256 devices in a mesh: grp: 2 (over y), sp: 32 (over z, core), tp: 4 (over x).
Axes of the slice: x: 4, y: 2, z: 16, core: 2. Of those that a mesh axis runs over, the one named last changes fastest.
The devices are a block of a 4x16x16 slice.
Arguments:
- residual_in: bfloat16 [20480, 2048], P(('grp', 'sp', 'tp')), parts along dimension 0, may hold values from -6 to 6
- narrow_query_rows: bfloat16 [20480, 1024], P(('grp', 'sp'), 'tp'), parts along dimension 0, may hold values from -5 to 5
- wide_query_rows: bfloat16 [20480, 1024], P(('grp', 'sp'), 'tp'), parts along dimension 0, may hold values from -5 to 5
- narrow_key_value: bfloat16 [20480, 4, 128], P(('grp', 'sp'), 'tp'), parts along dimension 0, may hold values from -120 to 120
- wide_key_value: bfloat16 [20480, 4, 256], P(('grp', 'sp'), 'tp'), parts along dimension 0, may hold values from -120 to 120
- narrow_norm_gains: float32 [2, 64], replicated, may hold values from 0.1 to 10
- wide_norm_gains: float32 [2, 128], replicated, may hold values from 0.1 to 10
- out_narrow: bfloat16 [1024, 2048], P('tp'), may hold values from -0.1875 to 0.1875
- out_wide: bfloat16 [1024, 2048], P('tp'), may hold values from -0.1875 to 0.1875
- mixer_gain: float32 [2048], replicated, may hold values from 0.1 to 1.9
- mixer_gate: bfloat16 [2048, 5632], P('sp', 'tp'), may hold values from -0.125 to 0.125
- mixer_up: bfloat16 [2048, 5632], P('sp', 'tp'), may hold values from -0.125 to 0.125
- mixer_down: bfloat16 [5632, 2048], P('tp', 'sp'), may hold values from -0.078125 to 0.078125
Outputs:
- layer_out: bfloat16 [20480, 2048], P(('grp', 'sp', 'tp')), parts along dimension 0
The draws below stay inside these ranges and needn't reach their ends.
There are 2 independent parts, one for each index of `grp`. The reference program is written for one: setup_inputs(seed, part) draws one part's arguments, and reference() takes and returns one part's arrays. A program takes and returns all parts, laid end to end along the dimension named above; an argument that names none is the same for every part. Nothing has to cross between parts.
All inputs are finite; a program needn't handle non-finite values.
Results may differ from the reference program's by a relative error of at most 0.015.
The reference program's roundings to bfloat16 on the way count: a program that leaves them out, or rounds other values in their place, can miss the bound.
Values may be sent and summed in bfloat16 or wider, within the bound.
A program may use at most 128 MiB of HBM per device.

```python
import math
import jax
import jax.numpy as jnp
from jax import lax

D = 2048
FF = 5632
NARROW_HEAD_SIZE = 64
WIDE_HEAD_SIZE = 128
NARROW_QUERIES = 16
NARROW_KEY_HEADS = 4
WIDE_QUERIES = 8
WIDE_KEY_HEADS = 4
GRID = 64
TOKENS = 10240
N_TP = 4


def plain_entries(key, shape):
    return jnp.clip(jax.random.normal(key, shape, jnp.float32), -5.0, 5.0)


def value_entries(key, shape):
    return jnp.clip(24.0 * jax.random.normal(key, shape, jnp.float32), -120.0, 120.0)


def group_keys(key, heads, width, salt):
    return plain_entries(jax.random.fold_in(key, salt), (TOKENS, heads, width))


def group_query_heads(key, heads, key_heads, width, salt):
    queries = plain_entries(jax.random.fold_in(key, salt + 1), (TOKENS, heads, width))
    return queries.reshape(TOKENS, heads * width)


def group_key_value(key, heads, width, salt):
    keys = group_keys(key, heads, width, salt)
    values = value_entries(jax.random.fold_in(key, salt + 2), (TOKENS, heads, width))
    return jnp.concatenate([keys, values], axis=-1)


def group_gains(key, width, salt):
    inner = jax.random.fold_in(key, salt)
    return jnp.clip(1.0 + 0.18 * jax.random.normal(inner, (2, width), jnp.float32), 0.1, 1.9)


def draw_narrow_query_rows(key, part):
    return group_query_heads(key, NARROW_QUERIES, NARROW_KEY_HEADS, NARROW_HEAD_SIZE, 100).astype(jnp.bfloat16)


def draw_wide_query_rows(key, part):
    return group_query_heads(key, WIDE_QUERIES, WIDE_KEY_HEADS, WIDE_HEAD_SIZE, 200).astype(jnp.bfloat16)


def draw_narrow_key_value(key, part):
    return group_key_value(key, NARROW_KEY_HEADS, NARROW_HEAD_SIZE, 100).astype(jnp.bfloat16)


def draw_wide_key_value(key, part):
    return group_key_value(key, WIDE_KEY_HEADS, WIDE_HEAD_SIZE, 200).astype(jnp.bfloat16)


def draw_narrow_norm_gains(key, part):
    return group_gains(key, NARROW_HEAD_SIZE, 300)


def draw_wide_norm_gains(key, part):
    return group_gains(key, WIDE_HEAD_SIZE, 400)


def level_of(stream_key, dims, split, low, top_value):
    def one(dim, blocks):
        heights = jax.random.uniform(jax.random.fold_in(jax.random.fold_in(stream_key, 6), dim), (blocks,), jnp.float32, low / len(split), top_value / len(split))
        return jnp.repeat(jnp.exp(heights), dims[dim] // blocks).reshape((-1,) + (1,) * (len(dims) - dim - 1))

    factor_of = one(*split[0])
    for cut in split[1:]:
        factor_of = factor_of * one(*cut)
    return factor_of


def scatter_about(key, extent, scale, bound, shards=(), kind=jnp.bfloat16):
    entries = scale * jax.random.normal(key, extent, jnp.float32)
    if shards:
        entries = entries * level_of(key, extent, shards, -0.22, 0.18)
    return jnp.clip(entries, -bound, bound).astype(kind)


def setup_inputs(seed: int = 0, part: int = 0) -> dict:
    key_list = jax.random.split(jax.random.key(seed), 14)
    own_keys = jax.random.split(jax.random.fold_in(key_list[13], part), 14)
    residual_in = scatter_about(own_keys[0], (TOKENS, D), 1.0, 6.0, ((0, 128),))
    narrow_query_rows = draw_narrow_query_rows(jax.random.fold_in(jax.random.fold_in(key_list[13], part), 71), part)
    wide_query_rows = draw_wide_query_rows(jax.random.fold_in(jax.random.fold_in(key_list[13], part), 71), part)
    narrow_key_value = draw_narrow_key_value(jax.random.fold_in(jax.random.fold_in(key_list[13], part), 71), part)
    wide_key_value = draw_wide_key_value(jax.random.fold_in(jax.random.fold_in(key_list[13], part), 71), part)
    narrow_norm_gains = draw_narrow_norm_gains(jax.random.fold_in(key_list[13], 71), part)
    wide_norm_gains = draw_wide_norm_gains(jax.random.fold_in(key_list[13], 71), part)
    out_narrow = scatter_about(key_list[7], (NARROW_QUERIES * NARROW_HEAD_SIZE, D), (NARROW_QUERIES * NARROW_HEAD_SIZE) ** -0.5, 0.1875, ((0, 4),))
    out_wide = scatter_about(key_list[8], (WIDE_QUERIES * WIDE_HEAD_SIZE, D), (WIDE_QUERIES * WIDE_HEAD_SIZE) ** -0.5, 0.1875, ((0, 4),))
    mixer_gain = jnp.clip(1.0 + 0.18 * jax.random.normal(key_list[9], (D,), jnp.float32), 0.1, 1.9)
    mixer_gate = scatter_about(key_list[10], (D, FF), D ** -0.5, 0.125, ((0, 32), (1, 4)))
    mixer_up = scatter_about(key_list[11], (D, FF), D ** -0.5, 0.125, ((0, 32), (1, 4)))
    mixer_down = scatter_about(key_list[12], (FF, D), FF ** -0.5, 0.078125, ((0, 4), (1, 32)))
    return {"residual_in": residual_in, "narrow_query_rows": narrow_query_rows, "wide_query_rows": wide_query_rows, "narrow_key_value": narrow_key_value, "wide_key_value": wide_key_value, "narrow_norm_gains": narrow_norm_gains, "wide_norm_gains": wide_norm_gains, "out_narrow": out_narrow, "out_wide": out_wide, "mixer_gain": mixer_gain, "mixer_gate": mixer_gate, "mixer_up": mixer_up, "mixer_down": mixer_down}


eps = 1e-06
theta = 10000.0

def rounded(value):
    return lax.optimization_barrier(value.astype(jnp.bfloat16)).astype(jnp.float32)

def grid_angles(width):
    positions = jnp.arange(TOKENS, dtype=jnp.int32)
    quarter = width // 4
    freqs = theta ** (-jnp.arange(quarter, dtype=jnp.float32) * 4.0 / width)
    row = (positions // GRID).astype(jnp.float32)
    column = (positions % GRID).astype(jnp.float32)
    return jnp.concatenate([row[:, None] * freqs[None, :], column[:, None] * freqs[None, :]], axis=-1)

def prepare(raw, gain, angles):
    field = raw.astype(jnp.float32)
    field = field * lax.rsqrt(lax.optimization_barrier(jnp.mean(field * field, axis=-1, keepdims=True)) + eps) * gain.astype(jnp.float32)
    half = field.shape[-1] // 2
    cosine = jnp.cos(angles)[:, None, :]
    sine = jnp.sin(angles)[:, None, :]
    first = field[..., :half]
    second = field[..., half:]
    turned = jnp.concatenate([first * cosine - second * sine, second * cosine + first * sine], axis=-1)
    return rounded(turned)

def attend_heads(query_raw, keyval, gains, heads, key_heads, width):
    angles = grid_angles(width)
    queries = prepare(query_raw.reshape(TOKENS, heads, width), gains[0], angles)
    keys = prepare(keyval[:, :, :width], gains[1], angles)
    values = keyval[:, :, width:].astype(jnp.float32)
    group = heads // key_heads
    block = math.gcd(TOKENS, 128)
    blocks = queries.reshape(TOKENS // block, block, key_heads, group, width)

    def one(piece):
        scores = jnp.einsum('qkgd,skd->kgqs', piece, keys) / math.sqrt(width)
        peak = lax.optimization_barrier(jnp.max(scores, axis=-1, keepdims=True))
        weights = jnp.exp(scores - peak)
        total = lax.optimization_barrier(jnp.sum(weights, axis=-1))
        summed = jnp.einsum('kgqs,skd->qkgd', rounded(weights), values)
        return (summed / jnp.transpose(total, (2, 0, 1))[..., None]).astype(jnp.bfloat16)
    result = lax.map(one, blocks)
    return result.reshape(TOKENS, heads * width)

def reference(residual_in, narrow_query_rows, wide_query_rows, narrow_key_value, wide_key_value, narrow_norm_gains, wide_norm_gains, out_narrow, out_wide, mixer_gain, mixer_gate, mixer_up, mixer_down):
    attention_narrow = attend_heads(narrow_query_rows, narrow_key_value, narrow_norm_gains, NARROW_QUERIES, NARROW_KEY_HEADS, NARROW_HEAD_SIZE)
    attention_wide = attend_heads(wide_query_rows, wide_key_value, wide_norm_gains, WIDE_QUERIES, WIDE_KEY_HEADS, WIDE_HEAD_SIZE)
    cols_narrow = NARROW_QUERIES * NARROW_HEAD_SIZE // N_TP
    cols_wide = WIDE_QUERIES * WIDE_HEAD_SIZE // N_TP
    attended = jnp.zeros((TOKENS, D), jnp.float32)
    for index in range(N_TP):
        lo_n = index * cols_narrow
        lo_w = index * cols_wide
        part = jnp.dot(attention_narrow[:, lo_n:lo_n + cols_narrow], out_narrow[lo_n:lo_n + cols_narrow], preferred_element_type=jnp.float32)
        part = part + jnp.dot(attention_wide[:, lo_w:lo_w + cols_wide], out_wide[lo_w:lo_w + cols_wide], preferred_element_type=jnp.float32)
        attended = attended + rounded(part)
    attended = attended.astype(jnp.bfloat16)
    stream = residual_in.astype(jnp.float32) + attended.astype(jnp.float32)
    scale = lax.rsqrt(lax.optimization_barrier(jnp.mean(stream * stream, axis=-1, keepdims=True)) + eps)
    normed = (stream * scale * mixer_gain.astype(jnp.float32)).astype(jnp.bfloat16)
    gate = jnp.dot(normed, mixer_gate, preferred_element_type=jnp.float32)
    up = jnp.dot(normed, mixer_up, preferred_element_type=jnp.float32)
    hidden = (jax.nn.silu(gate) * up).astype(jnp.bfloat16)
    units = FF // N_TP
    branch = jnp.zeros((TOKENS, D), jnp.float32)
    for index in range(N_TP):
        lo_u = index * units
        branch = branch + rounded(jnp.dot(hidden[:, lo_u:lo_u + units], mixer_down[lo_u:lo_u + units], preferred_element_type=jnp.float32))
    branch = branch.astype(jnp.bfloat16)
    return (stream + branch.astype(jnp.float32)).astype(jnp.bfloat16)
```

```python
import functools
import math

import jax
import jax.numpy as jnp
import numpy as np
from jax import lax
from jax.experimental import pallas as pl
from jax.experimental.pallas import tpu as pltpu
from jax.sharding import PartitionSpec as P

GRID = 64
EPS = 1e-06
THETA = 10000.0
MESH = pl.DeviceIdType.MESH
F32 = jnp.float32
BF16 = jnp.bfloat16
CHUNKS = 4
PAD = 16


def nt(a, b):
    return lax.dot_general(a, b, (((1,), (1,)), ((), ())), preferred_element_type=F32)


def nn(a, b):
    return jnp.dot(a, b, preferred_element_type=F32)


def turn_tables(start, tokens, width):
    quarter = width // 4
    freqs = THETA ** (-jnp.arange(quarter, dtype=F32) * 4.0 / width)
    positions = start + jnp.arange(tokens, dtype=jnp.int32)
    row = (positions // GRID).astype(F32)
    column = (positions % GRID).astype(F32)
    angles = jnp.concatenate([row[:, None] * freqs[None], column[:, None] * freqs[None]], axis=-1)
    cosine, sine = jnp.cos(angles), jnp.sin(angles)
    return jnp.concatenate([cosine, cosine, -sine, sine], axis=-1)


def prepared(raw, gain, table):
    width = raw.shape[1]
    field = raw.astype(F32)
    field = field * lax.rsqrt(jnp.mean(field * field, axis=-1, keepdims=True) + EPS) * gain
    swapped = jnp.concatenate([field[:, width // 2 :], field[:, : width // 2]], axis=1)
    return (field * table[:, :width] + swapped * table[:, width:]).astype(BF16)


class Group:
    def __init__(self, whole, queries, peak, summed, width, tile):
        self.whole, self.queries, self.peak, self.summed = whole, queries, peak, summed
        self.width, self.tile = width, tile

    def start(self):
        self.peak[...] = jnp.full(self.peak.shape, -1e30, F32)
        self.summed[...] = jnp.zeros(self.summed.shape, F32)

    def absorb(self, slot):
        width = self.width
        cores, tokens, columns = self.whole.shape[1:]
        block = self.whole[slot].reshape(cores * tokens, columns)
        if width % 128:
            keys, values = block, block.T[width:]
        else:
            keys, values = block[:, :width], block[:, width:].T
        ones = jnp.ones((PAD, cores * tokens), BF16)
        values = jnp.concatenate([ones, values], axis=0)
        factor = math.log2(math.e) / math.sqrt(width)
        total = self.queries.shape[0]
        for low in range(0, total, self.tile):
            span = slice(low, min(low + self.tile, total))
            scores = nt(keys, self.queries[span, :])
            old = self.peak[:, span]
            new = jnp.maximum(old, jnp.max(scores, axis=0, keepdims=True))
            self.peak[:, span] = new
            weights = jnp.exp2((scores - new) * factor).astype(BF16)
            rescale = jnp.exp2((old - new) * factor)
            self.summed[:, span] = self.summed[:, span] * rescale + nn(values, weights)

    def finished(self):
        result = self.summed[PAD:, :] / self.summed[0:1, :]
        return result.T.astype(BF16)


def reduce_scatter(dest, part, relay, pair, direct, sems, axis, emit):
    send_a, send_b, send_c, recv_a, recv_b, recv_c = sems
    me = lax.axis_index(axis)
    right, left = lax.rem(me + 1, 4), lax.rem(me + 3, 4)
    far = lax.rem(me + 2, 4)

    def ways(c):
        return (right, left) if c % 2 == 0 else (left, right)

    def first(c):
        ahead, behind = ways(c)
        return (
            pltpu.make_async_remote_copy(
                part.at[c, far], relay.at[c], send_a.at[c], recv_a.at[c], dest(ahead), MESH
            ),
            pltpu.make_async_remote_copy(
                part.at[c, behind], direct.at[c], send_b.at[c], recv_b.at[c], dest(behind), MESH
            ),
        )

    def second(c):
        ahead, _ = ways(c)
        return pltpu.make_async_remote_copy(
            pair.at[c, 0], pair.at[c, 1], send_c.at[c], recv_c.at[c], dest(ahead), MESH
        )

    def forward(c):
        first(c)[0].wait_recv()
        ahead, _ = ways(c)
        pair[c, 0] = (part[c, ahead].astype(F32) + relay[c].astype(F32)).astype(BF16)
        second(c).start()

    for c in range(CHUNKS):
        emit(c)
        for copy in first(c):
            copy.start()
        if c:
            forward(c - 1)
    forward(CHUNKS - 1)
    sums = []
    for c in range(CHUNKS):
        first(c)[1].wait_recv()
        second(c).wait_recv()
        total = part[c, me].astype(F32) + direct[c].astype(F32) + pair[c, 1].astype(F32)
        sums.append(total.astype(BF16))
    for c in range(CHUNKS):
        for copy in (*first(c), second(c)):
            copy.wait_send()
    return sums


def attention_kernel(
    chips,
    nq, wq, nkv, wkv, ngain, wgain, ntable, wtable, outw, residual, mgain,
    stream_out, rows_out,
    gn, gw, qn, qw, npeak, wpeak, nsum, wsum, attn, part, relay, pair, direct, rows,
    ring_send, ring_recv, mate_send, mate_recv,
    rs_sems, ag_send, ag_recv,
):
    sp, tp = lax.axis_index("sp"), lax.axis_index("tp")
    count = 2 * chips
    core = lax.rem(sp, 2)
    mate = sp + 1 - 2 * core
    up, down = lax.rem(sp + 2, count), lax.rem(sp + count - 2, count)
    right, left, across = lax.rem(tp + 1, 4), lax.rem(tp + 3, 4), lax.rem(tp + 2, 4)
    half = chips // 2
    tokens = nq.shape[0]
    nwidth, wwidth = ngain.shape[1], wgain.shape[1]

    barrier = pltpu.get_barrier_semaphore()
    for where in ({"sp": up}, {"sp": down}, {"sp": mate}, {"tp": right}, {"tp": left}):
        pl.semaphore_signal(barrier, inc=1, device_id=where, device_id_type=MESH)

    wholes = (gn, gw)

    def ring(piece, way, slot, target, here=None):
        whole = wholes[piece]
        return pltpu.make_async_remote_copy(
            whole.at[slot, core],
            whole.at[target, core],
            ring_send.at[piece, way, slot],
            ring_recv.at[piece, target],
            {"sp": up if way == 0 else down},
            MESH,
        )

    def to_mate(piece, slot):
        whole = wholes[piece]
        return pltpu.make_async_remote_copy(
            whole.at[slot, core],
            whole.at[slot, core],
            mate_send.at[piece, slot],
            mate_recv.at[piece, slot],
            {"sp": mate},
            MESH,
        )

    def arrive(piece, slot):
        ring(piece, 0, slot, slot).wait_recv()

    gn[0, core] = jnp.concatenate(
        [prepared(nkv[:, :nwidth], ngain[1:2, :], ntable[...]), nkv[:, nwidth:]], axis=1
    )
    gw[0, core, :, :wwidth] = prepared(wkv[:, :wwidth], wgain[1:2, :], wtable[...])
    gw[0, core, :, wwidth:] = wkv[:, wwidth:]
    pl.semaphore_wait(barrier, 5)
    for piece in (0, 1):
        ring(piece, 0, 0, 1).start()
        ring(piece, 1, 0, half + 1).start()
        to_mate(piece, 0).start()

    zeros = jnp.zeros((tokens, qn.shape[1] - nwidth), BF16)
    for head in range(qn.shape[0] // tokens):
        raw = nq[:, head * nwidth : (head + 1) * nwidth]
        turned = prepared(raw, ngain[0:1, :], ntable[...])
        qn[head * tokens : (head + 1) * tokens, :] = jnp.concatenate([turned, zeros], axis=1)
    for head in range(qw.shape[0] // tokens):
        raw = wq[:, head * wwidth : (head + 1) * wwidth]
        qw[head * tokens : (head + 1) * tokens, :] = prepared(raw, wgain[0:1, :], wtable[...])
    narrow = Group(gn, qn, npeak, nsum, nwidth, 256)
    wide = Group(gw, qw, wpeak, wsum, wwidth, 256)
    narrow.start()
    wide.start()
    groups = (narrow, wide)

    def absorb(piece, step):
        def one(i, carry):
            slot = jnp.where(i == 0, step, half + step)
            to_mate(piece, slot).wait_recv()
            groups[piece].absorb(slot)
            return carry

        lax.fori_loop(0, jnp.where((step == 0) | (step == half), 1, 2), one, 0)

    def pass_on(piece, step):
        @pl.when(step < half)
        def _():
            arrive(piece, step)
            if piece == 1:
                ring(piece, 0, step, step + 1).start()
            else:

                @pl.when(step + 1 < half)
                def _():
                    ring(piece, 0, step, step + 1).start()

            to_mate(piece, step).start()
            arrive(piece, half + step)
            if piece == 0:
                ring(piece, 1, half + step, jnp.where(step + 1 < half, half + step + 1, half)).start()
            else:

                @pl.when(step + 1 < half)
                def _():
                    ring(piece, 1, half + step, half + step + 1).start()

            to_mate(piece, half + step).start()

        @pl.when(step == half)
        def _():
            arrive(piece, half)
            to_mate(piece, half).start()

    absorb(0, jnp.int32(0))

    def turn(step, carry):
        pass_on(0, step)
        absorb(1, step - 1)
        pass_on(1, step)
        absorb(0, step)
        return carry

    lax.fori_loop(1, half + 1, turn, 0)
    absorb(1, jnp.int32(half))

    narrow_rows, wide_rows = narrow.finished(), wide.finished()
    low = 0
    for result, width in ((narrow_rows, nwidth), (wide_rows, wwidth)):
        for head in range(result.shape[0] // tokens):
            attn[:, low : low + width] = result[head * tokens : (head + 1) * tokens]
            low += width

    chunk = part.shape[3]

    def emit(c):
        terms = nn(attn[...], outw[:, c * chunk : (c + 1) * chunk]).astype(BF16)
        part[c] = terms.reshape(part.shape[1:])

    def dest(j):
        return {"tp": j}

    sums = reduce_scatter(dest, part, relay, pair, direct, rs_sems, "tp", emit)
    stream = residual[...].astype(F32) + jnp.concatenate(sums, axis=1).astype(F32)
    stream_out[...] = stream
    scale = lax.rsqrt(jnp.mean(stream * stream, axis=-1, keepdims=True) + EPS)
    normed = (stream * scale * mgain[...]).astype(BF16)
    split = rows.shape[3]
    rows[0, tp] = normed[:, :split]
    rows[1, tp] = normed[:, split:]

    def gather(h, way, owner):
        return pltpu.make_async_remote_copy(
            rows.at[h, owner],
            rows.at[h, owner],
            ag_send.at[h, way, owner],
            ag_recv.at[h, owner],
            {"tp": right if way == 0 else left},
            MESH,
        )

    gather(0, 0, tp).start()
    gather(1, 1, tp).start()
    gather(1, 0, tp).start()
    gather(0, 1, tp).start()
    gather(0, 0, left).wait_recv()
    gather(0, 0, left).start()
    gather(1, 0, right).wait_recv()
    gather(1, 1, right).start()
    for h, owner in ((1, left), (0, right), (0, across), (1, across)):
        gather(h, 0, owner).wait_recv()
    for h in (0, 1):
        rows_out[h] = rows[h].reshape(rows_out.shape[1:])
    for h, way, owner in ((0, 0, tp), (1, 1, tp), (1, 0, tp), (0, 1, tp), (0, 0, left), (1, 1, right)):
        gather(h, way, owner).wait_send()

    def drain(step, carry):
        for piece in (0, 1):

            @pl.when((step < half) if piece == 1 else (step + 1 < half))
            def _():
                ring(piece, 0, step, step + 1).wait_send()

            back = jnp.where(step == 0, 0, half + step)

            @pl.when((step < half) if piece == 0 else (step + 1 < half))
            def _():
                ring(piece, 1, back, half).wait_send()

            to_mate(piece, step).wait_send()

            @pl.when((step > 0) & (step < half))
            def _():
                to_mate(piece, half + step).wait_send()

        return carry

    lax.fori_loop(0, half + 1, drain, 0)


def mixer_kernel(
    rows, stream, weights,
    out,
    held, hidden, part, relay, pair, direct, fetch, rs_sems,
):
    tp = lax.axis_index("tp")
    right, left = lax.rem(tp + 1, 4), lax.rem(tp + 3, 4)
    barrier = pltpu.get_barrier_semaphore()
    for j in (right, left):
        pl.semaphore_signal(barrier, inc=1, device_id={"tp": j}, device_id_type=MESH)
    units = hidden.shape[1]
    split = rows.shape[2]

    def load(i):
        span = pl.ds(pl.multiple_of(i * 128, 128), 128)
        return pltpu.make_async_copy(weights.at[:, span], held.at[:, span], fetch.at[i])

    blocks = units // 128

    def begin(i, carry):
        load(i).start()
        load(blocks + i).start()
        return carry

    def begin_down(i, carry):
        load(2 * blocks + i).start()
        return carry

    lax.fori_loop(0, blocks, begin, 0)
    lax.fori_loop(0, blocks, begin_down, 0)

    def visit(i, carry):
        load(i).wait()
        load(blocks + i).wait()
        gates = pl.ds(pl.multiple_of(i * 128, 128), 128)
        ups = pl.ds(pl.multiple_of(units + i * 128, 128), 128)
        both = jnp.concatenate([held[:, gates], held[:, ups]], axis=1)
        product = nn(rows[0], both[:split]) + nn(rows[1], both[split:])
        gate, up = product[:, :128], product[:, 128:]
        hidden[:, gates] = (gate / (1.0 + jnp.exp(-gate)) * up).astype(BF16)
        return carry

    lax.fori_loop(0, blocks, visit, 0)

    def arrive(i, carry):
        load(2 * blocks + i).wait()
        return carry

    lax.fori_loop(0, blocks, arrive, 0)
    pl.semaphore_wait(barrier, 2)
    chunk = part.shape[3]

    def emit(c):
        terms = nt(hidden[...], held[c * chunk : (c + 1) * chunk, 2 * units :]).astype(BF16)
        part[c] = terms.reshape(part.shape[1:])

    def dest(j):
        return {"tp": j}

    sums = reduce_scatter(dest, part, relay, pair, direct, rs_sems, "tp", emit)
    out[...] = (stream[...] + jnp.concatenate(sums, axis=1).astype(F32)).astype(BF16)


def scatter_scratch(tokens, owned, chunk):
    return [
        pltpu.VMEM((CHUNKS, tokens // owned, owned, chunk), BF16),
        pltpu.VMEM((CHUNKS, owned, chunk), BF16),
        pltpu.VMEM((CHUNKS, 2, owned, chunk), BF16),
        pltpu.VMEM((CHUNKS, owned, chunk), BF16),
    ]


def scatter_sems():
    return [pltpu.SemaphoreType.DMA((CHUNKS,))] * 6


def local(
    chips,
    residual_in,
    narrow_query_rows,
    wide_query_rows,
    narrow_key_value,
    wide_key_value,
    narrow_norm_gains,
    wide_norm_gains,
    out_narrow,
    out_wide,
    mixer_gain,
    mixer_gate,
    mixer_up,
    mixer_down,
):
    shard = jnp.concatenate([mixer_gate, mixer_up, mixer_down.T], axis=1)
    weights = lax.all_gather(shard, "sp", axis=0, tiled=True)

    tokens = narrow_query_rows.shape[0]
    owned, model = residual_in.shape
    nkv = narrow_key_value.reshape(tokens, -1)
    wkv = wide_key_value.reshape(tokens, -1)
    nwidth, wwidth = nkv.shape[1] // 2, wkv.shape[1] // 2
    nrows = narrow_query_rows.shape[1] // nwidth * tokens
    wrows = wide_query_rows.shape[1] // wwidth * tokens
    start = lax.axis_index("sp") * tokens
    ntable = turn_tables(start, tokens, nwidth)
    wtable = turn_tables(start, tokens, wwidth)
    outw = jnp.concatenate([out_narrow, out_wide], axis=0)
    chunk = model // CHUNKS
    vmem = pl.BlockSpec(memory_space=pltpu.VMEM)
    DMA = pltpu.SemaphoreType.DMA

    stream, rows = pl.pallas_call(
        functools.partial(unpacked_attention, chips),
        out_shape=(
            jax.ShapeDtypeStruct((owned, model), F32),
            jax.ShapeDtypeStruct((2, tokens, model // 2), BF16),
        ),
        in_specs=[vmem] * 11,
        out_specs=(vmem, vmem),
        scratch_shapes=[
            pltpu.VMEM((chips, 2, tokens, nkv.shape[1]), BF16),
            pltpu.VMEM((chips, 2, tokens, wkv.shape[1]), BF16),
            pltpu.VMEM((nrows, nkv.shape[1]), BF16),
            pltpu.VMEM((wrows, wwidth), BF16),
            pltpu.VMEM((1, nrows), F32),
            pltpu.VMEM((1, wrows), F32),
            pltpu.VMEM((PAD + nwidth, nrows), F32),
            pltpu.VMEM((PAD + wwidth, wrows), F32),
            pltpu.VMEM((tokens, outw.shape[0]), BF16),
            *scatter_scratch(tokens, owned, chunk),
            pltpu.VMEM((2, tokens // owned, owned, model // 2), BF16),
            DMA((2, 2, chips)),
            DMA((2, chips)),
            DMA((2, chips)),
            DMA((2, chips)),
            *scatter_sems(),
            DMA((2, 2, tokens // owned)),
            DMA((2, tokens // owned)),
        ],
        compiler_params=pltpu.CompilerParams(
            collective_id=0, has_side_effects=True, vmem_limit_bytes=48 * 2**20
        ),
        cost_estimate=pl.CostEstimate(
            flops=60_000_000_000, bytes_accessed=10_000_000, transcendentals=20_000_000
        ),
        name="attend",
    )(
        narrow_query_rows,
        wide_query_rows,
        nkv,
        wkv,
        narrow_norm_gains,
        wide_norm_gains,
        ntable,
        wtable,
        outw,
        residual_in,
        mixer_gain.reshape(1, -1),
    )

    units = mixer_gate.shape[1]
    return pl.pallas_call(
        unpacked_mixer,
        out_shape=jax.ShapeDtypeStruct((owned, model), BF16),
        in_specs=[vmem, vmem, pl.BlockSpec(memory_space=pl.ANY)],
        out_specs=vmem,
        scratch_shapes=[
            pltpu.VMEM((model, 3 * units), BF16),
            pltpu.VMEM((tokens, units), BF16),
            *scatter_scratch(tokens, owned, chunk),
            DMA((3 * units // 128,)),
            *scatter_sems(),
        ],
        compiler_params=pltpu.CompilerParams(
            collective_id=1, has_side_effects=True, vmem_limit_bytes=48 * 2**20
        ),
        cost_estimate=pl.CostEstimate(
            flops=6_000_000_000, bytes_accessed=20_000_000, transcendentals=500_000
        ),
        name="mix",
    )(rows, stream, weights)


def unpacked_attention(chips, *refs):
    head, sems = refs[:31], refs[31:]
    attention_kernel(chips, *head, sems[0:6], sems[6], sems[7])


def unpacked_mixer(*refs):
    mixer_kernel(*refs[:11], refs[11:])


def solution(mesh):
    placed = (
        P(("grp", "sp", "tp"), None),
        P(("grp", "sp"), "tp"),
        P(("grp", "sp"), "tp"),
        P(("grp", "sp"), "tp", None),
        P(("grp", "sp"), "tp", None),
        P(),
        P(),
        P("tp", None),
        P("tp", None),
        P(),
        P("sp", "tp"),
        P("sp", "tp"),
        P("tp", "sp"),
    )
    return jax.shard_map(
        functools.partial(local, mesh.shape["sp"] // 2),
        mesh=mesh,
        in_specs=placed,
        out_specs=P(("grp", "sp", "tp"), None),
        check_vma=False,
    )
```

```python
import functools
import math

import jax
import jax.numpy as jnp
import numpy as np
from jax import lax
from jax.experimental import pallas as pl
from jax.experimental.pallas import tpu as pltpu
from jax.sharding import PartitionSpec as P

GRID = 64
EPS = 1e-06
THETA = 10000.0
MESH = pl.DeviceIdType.MESH
F32 = jnp.float32
BF16 = jnp.bfloat16
CHUNKS = 4
PAD = 16


def nt(a, b):
    return lax.dot_general(a, b, (((1,), (1,)), ((), ())), preferred_element_type=F32)


def nn(a, b):
    return jnp.dot(a, b, preferred_element_type=F32)


def frequencies(*widths):
    lanes, rows = [], []
    for width in widths:
        quarter = width // 4
        freqs = np.float32(THETA) ** (-np.arange(quarter, dtype=np.float32) * np.float32(4.0 / width))
        lanes += [freqs, freqs]
        rows += [np.ones(quarter), np.zeros(quarter)]
    lanes, rows = np.concatenate(lanes), np.concatenate(rows)
    spare = -len(lanes) % 128
    return np.pad(np.stack([lanes, rows]), ((0, 6), (0, spare))).astype(np.float32)


def prepared(raw, gain, table):
    width = raw.shape[1]
    field = raw.astype(F32)
    field = field * lax.rsqrt(jnp.mean(field * field, axis=-1, keepdims=True) + EPS) * gain
    swapped = jnp.concatenate([field[:, width // 2 :], field[:, : width // 2]], axis=1)
    return (field * table[:, :width] + swapped * table[:, width:]).astype(BF16)


class Group:
    def __init__(self, whole, queries, peak, summed, width, tile):
        self.whole, self.queries, self.peak, self.summed = whole, queries, peak, summed
        self.width, self.tile = width, tile

    def start(self):
        self.peak[...] = jnp.full(self.peak.shape, -1e30, F32)
        self.summed[...] = jnp.zeros(self.summed.shape, F32)

    def split(self, slot):
        width = self.width
        cores, tokens, columns = self.whole.shape[1:]
        block = self.whole[slot].reshape(cores * tokens, columns)
        if width % 128:
            keys, values = block, block.T[width:]
        else:
            keys, values = block[:, :width], block[:, width:].T
        ones = jnp.ones((PAD, cores * tokens), BF16)
        return keys, jnp.concatenate([ones, values], axis=0)

    def absorb(self, slots):
        factor = math.log2(math.e) / math.sqrt(self.width)
        total = self.queries.shape[0]
        spans = [slice(low, min(low + self.tile, total)) for low in range(0, total, self.tile)]
        items = [(block, span) for block in map(self.split, slots) for span in spans]

        def score(item):
            (keys, _), span = item
            return nt(keys, self.queries[span, :])

        def add(values, weights, rescale, span):
            self.summed[:, span] = self.summed[:, span] * rescale + nn(values, weights)

        behind = None
        ahead = score(items[0])
        for i, ((_, values), span) in enumerate(items):
            scores = ahead
            if i + 1 < len(items):
                ahead = score(items[i + 1])
            if behind is not None:
                add(*behind)
            old = self.peak[:, span]
            new = jnp.maximum(old, jnp.max(scores, axis=0, keepdims=True))
            self.peak[:, span] = new
            weights = jnp.exp2((scores - new) * factor).astype(BF16)
            behind = (values, weights, jnp.exp2((old - new) * factor), span)
        add(*behind)

    def finished(self):
        result = self.summed[PAD:, :] / self.summed[0:1, :]
        return result.T.astype(BF16)


def reduce_scatter(dest, part, relay, pair, direct, sems, axis, emit, serve):
    send_a, send_b, send_c, recv_a, recv_b, recv_c = sems
    me = lax.axis_index(axis)
    right, left = lax.rem(me + 1, 4), lax.rem(me + 3, 4)
    far = lax.rem(me + 2, 4)

    def ways(c):
        return (right, left) if c % 2 == 0 else (left, right)

    def relayed(c):
        return pltpu.make_async_remote_copy(
            part.at[c, far], relay.at[c], send_a.at[c], recv_a.at[c], dest(ways(c)[0]), MESH
        )

    def straight(c):
        ahead, behind = ways(c)
        return pltpu.make_async_remote_copy(
            part.at[c, behind], direct.at[c], send_b.at[c], recv_b.at[c], dest(behind), MESH
        )

    def paired(c):
        return pltpu.make_async_remote_copy(
            pair.at[c, 0], pair.at[c, 1], send_c.at[c], recv_c.at[c], dest(ways(c)[0]), MESH
        )

    for c in range(CHUNKS):
        emit(c)
        relayed(c).start()
        straight(c).start()
        serve()
    for c in range(CHUNKS):
        relayed(c).wait_recv()
        ahead, _ = ways(c)
        pair[c, 0] = (part[c, ahead].astype(F32) + relay[c].astype(F32)).astype(BF16)
        paired(c).start()
        serve()
    sums = []
    for c in range(CHUNKS):
        straight(c).wait_recv()
        paired(c).wait_recv()
        total = part[c, me].astype(F32) + direct[c].astype(F32) + pair[c, 1].astype(F32)
        sums.append(total.astype(BF16))
    for c in range(CHUNKS):
        relayed(c).wait_send()
        straight(c).wait_send()
        paired(c).wait_send()
    return sums


def layer_kernel(
    chips,
    nq, wq, nkv, wkv, ngain, wgain, freqs, residual, mgain, down_shard,
    outn, outw, gate_shard, up_shard,
    out,
    ntable, wtable, weights, gn, gw, qn, qw, npeak, wpeak, nsum, wsum, attn, projection,
    part, relay, pair, direct, rows, hidden,
    ring_send, ring_recv, mate_send, mate_recv,
    wring_send, wring_recv, wmate_send, wmate_recv, cross_send, cross_recv,
    fetch, ag_send, ag_recv,
    *scatter_sems,
):
    grp, sp, tp = lax.axis_index("grp"), lax.axis_index("sp"), lax.axis_index("tp")
    count = 2 * chips
    core = lax.rem(sp, 2)
    mate = sp + 1 - 2 * core
    parity = lax.rem(grp, 2)
    twin = grp + 1 - 2 * parity
    above, below = lax.rem(sp + 2, count), lax.rem(sp + count - 2, count)
    right, left, across = lax.rem(tp + 1, 4), lax.rem(tp + 3, 4), lax.rem(tp + 2, 4)
    half = chips // 2
    tokens = nq.shape[0]
    nwidth, wwidth = ngain.shape[1], wgain.shape[1]

    barrier = pltpu.get_barrier_semaphore()
    greeted = ({"sp": above}, {"sp": below}, {"sp": mate}, {"tp": right}, {"tp": left}, {"grp": twin})
    for where in greeted:
        pl.semaphore_signal(barrier, inc=1, device_id=where, device_id_type=MESH)
    nrows = outn.shape[0]
    loads = (
        pltpu.make_async_copy(gate_shard, weights.at[0, sp], fetch.at[0]),
        pltpu.make_async_copy(up_shard, weights.at[1, sp], fetch.at[1]),
        pltpu.make_async_copy(down_shard, weights.at[2, sp], fetch.at[2]),
        pltpu.make_async_copy(outn, projection.at[:nrows], fetch.at[3]),
        pltpu.make_async_copy(outw, projection.at[nrows:], fetch.at[4]),
    )
    for copy in loads:
        copy.start()

    wholes = (gn, gw)

    def ring(piece, way, slot, target):
        whole = wholes[piece]
        return pltpu.make_async_remote_copy(
            whole.at[slot, core],
            whole.at[target, core],
            ring_send.at[piece, way, slot],
            ring_recv.at[piece, target],
            {"sp": above if way == 0 else below},
            MESH,
        )

    def to_mate(piece, slot):
        whole = wholes[piece]
        return pltpu.make_async_remote_copy(
            whole.at[slot, core],
            whole.at[slot, core],
            mate_send.at[piece, slot],
            mate_recv.at[piece, slot],
            {"sp": mate},
            MESH,
        )

    def arrive(piece, slot):
        ring(piece, 0, slot, slot).wait_recv()

    share = (parity, 2, 1 - parity)

    def source(slot):
        back = jnp.where(slot <= half, count - 2 * slot, 2 * (slot - half))
        return lax.rem(sp + back, count)

    def wring(kind, way, slot, target):
        block = weights.at[share[kind], source(slot)]
        return pltpu.make_async_remote_copy(
            block,
            block,
            wring_send.at[kind, way, slot],
            wring_recv.at[kind, target],
            {"sp": above if way == 0 else below},
            MESH,
        )

    def wmate(kind, slot):
        block = weights.at[share[kind], source(slot)]
        return pltpu.make_async_remote_copy(
            block, block, wmate_send.at[kind, slot], wmate_recv.at[kind, slot], {"sp": mate}, MESH
        )

    def cross(slot):
        block = weights.at[share[0], source(slot)]
        return pltpu.make_async_remote_copy(
            block, block, cross_send.at[slot], cross_recv.at[slot], {"grp": twin}, MESH
        )

    def serve_share(step, last=False):
        wring(0, 0, step, step).wait_recv()
        if not last:
            wring(0, 0, step, step + 1).start()
        cross(step).start()
        wmate(0, step).start()
        if last:
            return
        wring(0, 0, half + step, half + step).wait_recv()
        if not (isinstance(step, int) and step + 1 == half):
            wring(0, 1, half + step, half + step + 1).start()
        cross(half + step).start()
        wmate(0, half + step).start()

    def serve_down(step):
        wring(1, 0, step, step).wait_recv()
        if step + 1 < half:
            wring(1, 0, step, step + 1).start()
        wmate(1, step).start()
        if step < half:
            wring(1, 0, half + step, half + step).wait_recv()
            wring(1, 1, half + step, half + step + 1 if step + 1 < half else half).start()
            wmate(1, half + step).start()

    def serve_cross(step):
        cross(step).wait_recv()
        wmate(2, step).start()
        if step < half:
            cross(half + step).wait_recv()
            wmate(2, half + step).start()

    positions = sp * tokens + lax.broadcasted_iota(jnp.int32, (tokens, freqs.shape[1]), 0)
    grid_row = (positions // GRID).astype(F32)
    grid_column = (positions % GRID).astype(F32)
    angles = jnp.where(freqs[1:2, :] > 0.5, grid_row, grid_column) * freqs[0:1, :]
    cosine, sine = jnp.cos(angles), jnp.sin(angles)
    first = 0
    for table, width in ((wtable, wwidth), (ntable, nwidth)):
        c, z = (x[:, first : first + width // 2] for x in (cosine, sine))
        table[...] = jnp.concatenate([c, c, -z, z], axis=1)
        first += width // 2
    gn[0, core] = jnp.concatenate(
        [prepared(nkv[:, :nwidth], ngain[1:2, :], ntable[...]), nkv[:, nwidth:]], axis=1
    )
    gw[0, core, :, :wwidth] = prepared(wkv[:, :wwidth], wgain[1:2, :], wtable[...])
    gw[0, core, :, wwidth:] = wkv[:, wwidth:]
    pl.semaphore_wait(barrier, len(greeted))
    for piece in (0, 1):
        ring(piece, 0, 0, 1).start()
        ring(piece, 1, 0, half + 1).start()
        to_mate(piece, 0).start()
    for copy in loads[:2]:
        copy.wait()
    wring(0, 0, 0, 1).start()
    wring(0, 1, 0, half + 1).start()
    wmate(0, 0).start()
    wmate(2, 0).start()

    zeros = jnp.zeros((tokens, qn.shape[1] - nwidth), BF16)
    for head in range(qn.shape[0] // tokens):
        raw = nq[:, head * nwidth : (head + 1) * nwidth]
        turned = prepared(raw, ngain[0:1, :], ntable[...])
        qn[head * tokens : (head + 1) * tokens, :] = jnp.concatenate([turned, zeros], axis=1)
    for head in range(qw.shape[0] // tokens):
        raw = wq[:, head * wwidth : (head + 1) * wwidth]
        qw[head * tokens : (head + 1) * tokens, :] = prepared(raw, wgain[0:1, :], wtable[...])
    narrow = Group(gn, qn, npeak, nsum, nwidth, 256)
    wide = Group(gw, qw, wpeak, wsum, wwidth, 256)
    narrow.start()
    wide.start()
    groups = (narrow, wide)
    for copy in loads[2:]:
        copy.wait()

    def absorb(piece, *slots):
        for slot in slots:
            to_mate(piece, slot).wait_recv()
        groups[piece].absorb(slots)

    def pass_on(piece, step):
        @pl.when(step < half)
        def _():
            arrive(piece, step)
            if piece == 1:
                ring(piece, 0, step, step + 1).start()
            else:

                @pl.when(step + 1 < half)
                def _():
                    ring(piece, 0, step, step + 1).start()

            to_mate(piece, step).start()
            arrive(piece, half + step)
            if piece == 0:
                ring(piece, 1, half + step, jnp.where(step + 1 < half, half + step + 1, half)).start()
            else:

                @pl.when(step + 1 < half)
                def _():
                    ring(piece, 1, half + step, half + step + 1).start()

            to_mate(piece, half + step).start()

        @pl.when(step == half)
        def _():
            arrive(piece, half)
            to_mate(piece, half).start()

    absorb(0, 0)
    absorb(1, 0)
    early = half // 2

    def turn(step, carry):
        pass_on(0, step)

        @pl.when(step > 1)
        def _():
            absorb(1, step - 1, half + step - 1)

        pass_on(1, step)

        @pl.when(lax.rem(step, 2) == 0)
        def _():
            serve_share(step // 2)

        absorb(0, step, half + step)
        return carry

    lax.fori_loop(1, half, turn, 0)
    pass_on(0, jnp.int32(half))
    absorb(1, half - 1, chips - 1)
    pass_on(1, jnp.int32(half))
    serve_share(early)
    absorb(0, half)

    def begin_down():
        wring(1, 0, 0, 1).start()
        wring(1, 1, 0, half + 1).start()
        wmate(1, 0).start()

    events = [functools.partial(serve_share, early + 1), functools.partial(begin_down)]
    shares = [functools.partial(serve_share, k, k == half) for k in range(early + 2, half + 1)]
    crosses = [functools.partial(serve_cross, k) for k in range(1, half + 1)]
    downs = [functools.partial(serve_down, k) for k in range(1, half + 1)]
    order = "xcxcccxcdcdcddcdcddd"
    lanes = {"x": shares, "c": crosses, "d": downs}
    for letter in order:
        if lanes[letter]:
            events.append(lanes[letter].pop(0))
    for left_over in lanes.values():
        events.extend(left_over)

    def serve():
        if events:
            events.pop(0)()

    absorb(1, half)
    serve()
    serve()

    narrow_rows, wide_rows = narrow.finished(), wide.finished()
    low = 0
    for result, width in ((narrow_rows, nwidth), (wide_rows, wwidth)):
        for head in range(result.shape[0] // tokens):
            attn[:, low : low + width] = result[head * tokens : (head + 1) * tokens]
            low += width

    chunk = part.shape[3]

    def emit(c):
        terms = nn(attn[...], projection[:, c * chunk : (c + 1) * chunk]).astype(BF16)
        part[c] = terms.reshape(part.shape[1:])

    def dest(j):
        return {"tp": j}

    first, second = scatter_sems[:6], scatter_sems[6:]
    sums = reduce_scatter(dest, part.at[0:CHUNKS], relay.at[0], pair.at[0], direct.at[0], first, "tp", emit, serve)
    stream = residual[...].astype(F32) + jnp.concatenate(sums, axis=1).astype(F32)
    scale = lax.rsqrt(jnp.mean(stream * stream, axis=-1, keepdims=True) + EPS)
    normed = (stream * scale * mgain[...]).astype(BF16)
    split = rows.shape[3]
    rows[0, tp] = normed[:, :split]
    rows[1, tp] = normed[:, split:]

    def gather(h, way, owner):
        return pltpu.make_async_remote_copy(
            rows.at[h, owner],
            rows.at[h, owner],
            ag_send.at[h, way, owner],
            ag_recv.at[h, owner],
            {"tp": right if way == 0 else left},
            MESH,
        )

    gather(0, 0, tp).start()
    gather(1, 1, tp).start()
    gather(1, 0, tp).start()
    gather(0, 1, tp).start()
    serve()
    serve()
    gather(0, 0, left).wait_recv()
    gather(0, 0, left).start()
    gather(1, 0, right).wait_recv()
    gather(1, 1, right).start()
    serve()
    serve()
    for h, owner in ((1, left), (0, right), (0, across), (1, across)):
        gather(h, 0, owner).wait_recv()
        serve()

    def settle(kind):
        def one(slot, carry):
            wmate(kind, slot).wait_recv()
            return carry

        lax.fori_loop(0, chips, one, 0)

    keep = [f for f in events if f.func is not serve_down]
    later = [f for f in events if f.func is serve_down]
    events[:] = []
    for event in keep:
        event()
        if later:
            later.pop(0)()
    settle(0)
    settle(2)
    units = hidden.shape[1]
    model = weights.shape[1] * weights.shape[2]
    def visit(i, carry):
        span = pl.ds(pl.multiple_of(i * 128, 128), 128)
        both = [weights[k, :, :, span].reshape(model, 128) for k in (0, 1)]
        both = jnp.concatenate(both, axis=1)
        product = nn(rows[0].reshape(tokens, split), both[:split])
        product += nn(rows[1].reshape(tokens, split), both[split:])
        gate, up = product[:, :128], product[:, 128:]
        hidden[:, span] = (gate / (1.0 + jnp.exp(-gate)) * up).astype(BF16)
        return carry

    lax.fori_loop(0, units // 128, visit, 0)
    for event in later:
        event()
    settle(1)

    def emit_down(c):
        count_here = chunk // weights.shape[2]
        block = weights[2, c * count_here : (c + 1) * count_here].reshape(chunk, units)
        terms = nt(hidden[...], block).astype(BF16)
        part[CHUNKS + c] = terms.reshape(part.shape[1:])

    sums = reduce_scatter(
        dest, part.at[CHUNKS:], relay.at[1], pair.at[1], direct.at[1], second, "tp", emit_down, lambda: None
    )
    out[...] = (stream + jnp.concatenate(sums, axis=1).astype(F32)).astype(BF16)

    for h, way, owner in ((0, 0, tp), (1, 1, tp), (1, 0, tp), (0, 1, tp), (0, 0, left), (1, 1, right)):
        gather(h, way, owner).wait_send()

    def drain(step, carry):
        back = jnp.where(step == 0, 0, half + step)

        @pl.when(step < half)
        def _():
            ring(1, 0, step, step + 1).wait_send()
            ring(0, 1, back, half).wait_send()
            wring(0, 0, step, step + 1).wait_send()
            wring(1, 1, back, half).wait_send()

        @pl.when(step + 1 < half)
        def _():
            ring(0, 0, step, step + 1).wait_send()
            ring(1, 1, back, half).wait_send()
            wring(1, 0, step, step + 1).wait_send()
            wring(0, 1, back, half).wait_send()

        return carry

    lax.fori_loop(0, half + 1, drain, 0)

    def drain_slots(slot, carry):
        for piece in (0, 1):
            to_mate(piece, slot).wait_send()
        for kind in (0, 1, 2):
            wmate(kind, slot).wait_send()

        @pl.when(slot > 0)
        def _():
            cross(slot).wait_send()

        return carry

    lax.fori_loop(0, chips, drain_slots, 0)


def local(
    chips,
    residual_in,
    narrow_query_rows,
    wide_query_rows,
    narrow_key_value,
    wide_key_value,
    narrow_norm_gains,
    wide_norm_gains,
    out_narrow,
    out_wide,
    mixer_gain,
    mixer_gate,
    mixer_up,
    mixer_down,
):
    tokens = narrow_query_rows.shape[0]
    owned, model = residual_in.shape
    owners = tokens // owned
    nkv = narrow_key_value.reshape(tokens, -1)
    wkv = wide_key_value.reshape(tokens, -1)
    nwidth, wwidth = nkv.shape[1] // 2, wkv.shape[1] // 2
    nrows = narrow_query_rows.shape[1] // nwidth * tokens
    wrows = wide_query_rows.shape[1] // wwidth * tokens
    depth, units = mixer_gate.shape
    chunk = model // CHUNKS
    joint = out_narrow.shape[0] + out_wide.shape[0]
    vmem = pl.BlockSpec(memory_space=pltpu.VMEM)
    hbm = pl.BlockSpec(memory_space=pl.ANY)
    VMEM, DMA = pltpu.VMEM, pltpu.SemaphoreType.DMA

    return pl.pallas_call(
        functools.partial(layer_kernel, chips),
        out_shape=jax.ShapeDtypeStruct((owned, model), BF16),
        in_specs=[vmem] * 9 + [hbm] * 5,
        out_specs=vmem,
        scratch_shapes=[
            VMEM((tokens, 2 * nwidth), F32),
            VMEM((tokens, 2 * wwidth), F32),
            VMEM((3, 2 * chips, depth, units), BF16),
            VMEM((chips, 2, tokens, nkv.shape[1]), BF16),
            VMEM((chips, 2, tokens, wkv.shape[1]), BF16),
            VMEM((nrows, nkv.shape[1]), BF16),
            VMEM((wrows, wwidth), BF16),
            VMEM((1, nrows), F32),
            VMEM((1, wrows), F32),
            VMEM((PAD + nwidth, nrows), F32),
            VMEM((PAD + wwidth, wrows), F32),
            VMEM((tokens, joint), BF16),
            VMEM((joint, model), BF16),
            VMEM((2 * CHUNKS, owners, owned, chunk), BF16),
            VMEM((2, CHUNKS, owned, chunk), BF16),
            VMEM((2, CHUNKS, 2, owned, chunk), BF16),
            VMEM((2, CHUNKS, owned, chunk), BF16),
            VMEM((2, owners, owned, model // 2), BF16),
            VMEM((tokens, units), BF16),
            DMA((2, 2, chips)),
            DMA((2, chips)),
            DMA((2, chips)),
            DMA((2, chips)),
            DMA((2, 2, chips)),
            DMA((2, chips)),
            DMA((3, chips)),
            DMA((3, chips)),
            DMA((chips,)),
            DMA((chips,)),
            DMA((5,)),
            DMA((2, 2, owners)),
            DMA((2, owners)),
            *[DMA((CHUNKS,))] * 12,
        ],
        compiler_params=pltpu.CompilerParams(
            collective_id=0, has_side_effects=True, vmem_limit_bytes=60 * 2**20
        ),
        name="layer",
    )(
        narrow_query_rows,
        wide_query_rows,
        nkv,
        wkv,
        narrow_norm_gains,
        wide_norm_gains,
        jnp.asarray(frequencies(wwidth, nwidth)),
        residual_in,
        mixer_gain.reshape(1, -1),
        mixer_down.T,
        out_narrow,
        out_wide,
        mixer_gate,
        mixer_up,
    )


def solution(mesh):
    placed = (
        P(("grp", "sp", "tp"), None),
        P(("grp", "sp"), "tp"),
        P(("grp", "sp"), "tp"),
        P(("grp", "sp"), "tp", None),
        P(("grp", "sp"), "tp", None),
        P(),
        P(),
        P("tp", None),
        P("tp", None),
        P(),
        P("sp", "tp"),
        P("sp", "tp"),
        P("tp", "sp"),
    )
    return jax.shard_map(
        functools.partial(local, mesh.shape["sp"] // 2),
        mesh=mesh,
        in_specs=placed,
        out_specs=P(("grp", "sp", "tp"), None),
        check_vma=False,
    )
```

```python
import functools
import math

import jax
import jax.numpy as jnp
import numpy as np
from jax import lax
from jax.experimental import pallas as pl
from jax.experimental.pallas import tpu as pltpu
from jax.sharding import PartitionSpec as P

GRID = 64
EPS = 1e-06
THETA = 10000.0
MESH = pl.DeviceIdType.MESH
F32 = jnp.float32
BF16 = jnp.bfloat16
CHUNKS = 4
LATE_CHUNKS = 8
PAD = 16


def nt(a, b):
    return lax.dot_general(a, b, (((1,), (1,)), ((), ())), preferred_element_type=F32)


def nn(a, b):
    return jnp.dot(a, b, preferred_element_type=F32)


def frequencies(*widths):
    lanes, rows = [], []
    for width in widths:
        quarter = width // 4
        freqs = np.float32(THETA) ** (-np.arange(quarter, dtype=np.float32) * np.float32(4.0 / width))
        lanes += [freqs, freqs]
        rows += [np.ones(quarter), np.zeros(quarter)]
    lanes, rows = np.concatenate(lanes), np.concatenate(rows)
    spare = -len(lanes) % 128
    return np.pad(np.stack([lanes, rows]), ((0, 6), (0, spare))).astype(np.float32)


def prepared(raw, gain, table):
    width = raw.shape[1]
    field = raw.astype(F32)
    field = field * lax.rsqrt(jnp.mean(field * field, axis=-1, keepdims=True) + EPS) * gain
    swapped = jnp.concatenate([field[:, width // 2 :], field[:, : width // 2]], axis=1)
    return (field * table[:, :width] + swapped * table[:, width:]).astype(BF16)


class Group:
    def __init__(self, whole, queries, peak, summed, width, tile):
        self.whole, self.queries, self.peak, self.summed = whole, queries, peak, summed
        self.width, self.tile = width, tile

    def start(self):
        self.peak[...] = jnp.full(self.peak.shape, -1e30, F32)
        self.summed[...] = jnp.zeros(self.summed.shape, F32)

    def split(self, slot):
        width = self.width
        cores, tokens, columns = self.whole.shape[1:]
        block = self.whole[slot].reshape(cores * tokens, columns)
        if width % 128:
            keys, values = block, block.T[width:]
        else:
            keys, values = block[:, :width], block[:, width:].T
        ones = jnp.ones((PAD, cores * tokens), BF16)
        return keys, jnp.concatenate([ones, values], axis=0)

    def absorb(self, slots):
        factor = math.log2(math.e) / math.sqrt(self.width)
        total = self.queries.shape[0]
        spans = [slice(low, min(low + self.tile, total)) for low in range(0, total, self.tile)]
        items = [(block, span) for block in map(self.split, slots) for span in spans]

        def score(item):
            (keys, _), span = item
            return nt(keys, self.queries[span, :])

        def add(values, weights, rescale, span):
            self.summed[:, span] = self.summed[:, span] * rescale + nn(values, weights)

        behind = None
        ahead = score(items[0])
        for i, ((_, values), span) in enumerate(items):
            scores = ahead
            if i + 1 < len(items):
                ahead = score(items[i + 1])
            if behind is not None:
                add(*behind)
            old = self.peak[:, span]
            new = jnp.maximum(old, jnp.max(scores, axis=0, keepdims=True))
            self.peak[:, span] = new
            weights = jnp.exp2((scores - new) * factor).astype(BF16)
            behind = (values, weights, jnp.exp2((old - new) * factor), span)
        add(*behind)

    def finished(self):
        result = self.summed[PAD:, :] / self.summed[0:1, :]
        return result.T.astype(BF16)


def reduce_scatter(dest, buffers, sems, axis, emit, serve, finish, lag):
    part, relay, pair, direct = buffers
    send_a, send_b, send_c, recv_a, recv_b, recv_c = sems
    me = lax.axis_index(axis)
    right, left = lax.rem(me + 1, 4), lax.rem(me + 3, 4)
    far = lax.rem(me + 2, 4)

    def ways(c):
        return (right, left) if c % 2 == 0 else (left, right)

    def relayed(c):
        return pltpu.make_async_remote_copy(
            part.at[c, far], relay.at[c], send_a.at[c], recv_a.at[c], dest(ways(c)[0]), MESH
        )

    def straight(c):
        ahead, behind = ways(c)
        return pltpu.make_async_remote_copy(
            part.at[c, behind], direct.at[c], send_b.at[c], recv_b.at[c], dest(behind), MESH
        )

    def paired(c):
        return pltpu.make_async_remote_copy(
            pair.at[c, 0], pair.at[c, 1], send_c.at[c], recv_c.at[c], dest(ways(c)[0]), MESH
        )

    def forward(c):
        relayed(c).wait_recv()
        ahead, _ = ways(c)
        pair[c, 0] = (part[c, ahead].astype(F32) + relay[c].astype(F32)).astype(BF16)
        paired(c).start()

    chunks = part.shape[0]
    for c in range(chunks):
        emit(c)
        relayed(c).start()
        straight(c).start()
        serve()
        if c >= lag:
            forward(c - lag)
    for c in range(chunks - lag, chunks):
        forward(c)
        serve()
    for c in range(chunks):
        straight(c).wait_recv()
        paired(c).wait_recv()
        total = part[c, me].astype(F32) + direct[c].astype(F32) + pair[c, 1].astype(F32)
        finish(c, total.astype(BF16))
    for c in range(chunks):
        relayed(c).wait_send()
        straight(c).wait_send()
        paired(c).wait_send()


def layer_kernel(
    chips,
    nq, wq, nkv, wkv, ngain, wgain, freqs, residual, mgain, down_shard,
    outn, outw, gate_shard, up_shard,
    out,
    ntable, wtable, weights, gn, gw, qn, qw, npeak, wpeak, nsum, wsum, attn, projection,
    part, relay, pair, direct, part2, relay2, pair2, direct2, stream, rows, hidden,
    ring_send, ring_recv, mate_send, mate_recv,
    wring_send, wring_recv, wmate_send, wmate_recv, cross_send, cross_recv,
    fetch, ag_send, ag_recv,
    *scatter_sems,
):
    grp, sp, tp = lax.axis_index("grp"), lax.axis_index("sp"), lax.axis_index("tp")
    count = 2 * chips
    core = lax.rem(sp, 2)
    mate = sp + 1 - 2 * core
    parity = lax.rem(grp, 2)
    twin = grp + 1 - 2 * parity
    above, below = lax.rem(sp + 2, count), lax.rem(sp + count - 2, count)
    right, left, across = lax.rem(tp + 1, 4), lax.rem(tp + 3, 4), lax.rem(tp + 2, 4)
    half = chips // 2
    tokens = nq.shape[0]
    nwidth, wwidth = ngain.shape[1], wgain.shape[1]

    barrier = pltpu.get_barrier_semaphore()
    greeted = ({"sp": above}, {"sp": below}, {"sp": mate}, {"tp": right}, {"tp": left}, {"grp": twin})
    for where in greeted:
        pl.semaphore_signal(barrier, inc=1, device_id=where, device_id_type=MESH)
    nrows = outn.shape[0]
    loads = (
        pltpu.make_async_copy(gate_shard, weights.at[0, sp], fetch.at[0]),
        pltpu.make_async_copy(up_shard, weights.at[1, sp], fetch.at[1]),
        pltpu.make_async_copy(down_shard, weights.at[2, sp], fetch.at[2]),
        pltpu.make_async_copy(outn, projection.at[:nrows], fetch.at[3]),
        pltpu.make_async_copy(outw, projection.at[nrows:], fetch.at[4]),
    )
    for copy in loads:
        copy.start()

    wholes = (gn, gw)

    def sent(way, slot):
        return slot if way == 0 else jnp.where(slot == 0, half, slot)

    def ring(piece, way, slot, target):
        whole = wholes[piece]
        return pltpu.make_async_remote_copy(
            whole.at[slot, core],
            whole.at[target, core],
            ring_send.at[piece, sent(way, slot)],
            ring_recv.at[piece, target],
            {"sp": above if way == 0 else below},
            MESH,
        )

    def to_mate(piece, slot):
        whole = wholes[piece]
        return pltpu.make_async_remote_copy(
            whole.at[slot, core],
            whole.at[slot, core],
            mate_send.at[piece, slot],
            mate_recv.at[piece, slot],
            {"sp": mate},
            MESH,
        )

    def arrive(piece, slot):
        ring(piece, 0, slot, slot).wait_recv()

    share = (parity, 2, 1 - parity)

    def source(slot):
        back = jnp.where(slot <= half, count - 2 * slot, 2 * (slot - half))
        return lax.rem(sp + back, count)

    def wring(kind, part, way, slot, target):
        depth = weights.shape[2] // 2
        block = weights.at[share[kind], source(slot), pl.ds(part * depth, depth)]
        return pltpu.make_async_remote_copy(
            block,
            block,
            wring_send.at[kind, part, sent(way, slot)],
            wring_recv.at[kind, part, target],
            {"sp": above if way == 0 else below},
            MESH,
        )

    def wsend(kind):
        for part in (0, 1):
            wring(kind, part, 0, 0, 1).start()
            wring(kind, part, 1, 0, half + 1).start()
        wmate(kind, 0).start()

    def wpass(kind, step):
        if isinstance(step, int) and step == half:
            for part in (0, 1):
                wring(kind, part, 0, step, step).wait_recv()
            return
        final = isinstance(step, int) and step + 1 == half
        for part in (0, 1):
            wring(kind, part, 0, step, step).wait_recv()
            if not final or part == 0:
                wring(kind, part, 0, step, step + 1).start()
            wring(kind, part, 0, half + step, half + step).wait_recv()
            if not final:
                wring(kind, part, 1, half + step, half + step + 1).start()
            elif part == 1:
                wring(kind, part, 1, half + step, half).start()

    def wmate(kind, slot):
        block = weights.at[share[kind], source(slot)]
        return pltpu.make_async_remote_copy(
            block, block, wmate_send.at[kind, slot], wmate_recv.at[kind, slot], {"sp": mate}, MESH
        )

    def cross(slot):
        block = weights.at[share[0], source(slot)]
        return pltpu.make_async_remote_copy(
            block, block, cross_send.at[slot], cross_recv.at[slot], {"grp": twin}, MESH
        )

    def slots_of(step):
        return (step,) if isinstance(step, int) and step == half else (step, half + step)

    def serve_share(step):
        wpass(0, step)
        for slot in slots_of(step):
            cross(slot).start()
            wmate(0, slot).start()

    def serve_down(step):
        wpass(1, step)
        for slot in slots_of(step):
            wmate(1, slot).start()

    def serve_cross(step):
        cross(step).wait_recv()
        wmate(2, step).start()
        if step < half:
            cross(half + step).wait_recv()
            wmate(2, half + step).start()

    pl.semaphore_wait(barrier, len(greeted))
    for copy in loads[:2]:
        copy.wait()
    wsend(0)
    wmate(2, 0).start()
    positions = sp * tokens + lax.broadcasted_iota(jnp.int32, (tokens, freqs.shape[1]), 0)
    grid_row = (positions // GRID).astype(F32)
    grid_column = (positions % GRID).astype(F32)
    angles = jnp.where(freqs[1:2, :] > 0.5, grid_row, grid_column) * freqs[0:1, :]
    cosine, sine = jnp.cos(angles), jnp.sin(angles)
    first = 0
    for table, width in ((wtable, wwidth), (ntable, nwidth)):
        c, z = (x[:, first : first + width // 2] for x in (cosine, sine))
        table[...] = jnp.concatenate([c, c, -z, z], axis=1)
        first += width // 2
    gn[0, core] = jnp.concatenate(
        [prepared(nkv[:, :nwidth], ngain[1:2, :], ntable[...]), nkv[:, nwidth:]], axis=1
    )
    gw[0, core, :, :wwidth] = prepared(wkv[:, :wwidth], wgain[1:2, :], wtable[...])
    gw[0, core, :, wwidth:] = wkv[:, wwidth:]
    for piece in (0, 1):
        ring(piece, 0, 0, 1).start()
        ring(piece, 1, 0, half + 1).start()
        to_mate(piece, 0).start()

    zeros = jnp.zeros((tokens, qn.shape[1] - nwidth), BF16)
    for head in range(qn.shape[0] // tokens):
        raw = nq[:, head * nwidth : (head + 1) * nwidth]
        turned = prepared(raw, ngain[0:1, :], ntable[...])
        qn[head * tokens : (head + 1) * tokens, :] = jnp.concatenate([turned, zeros], axis=1)
    for head in range(qw.shape[0] // tokens):
        raw = wq[:, head * wwidth : (head + 1) * wwidth]
        qw[head * tokens : (head + 1) * tokens, :] = prepared(raw, wgain[0:1, :], wtable[...])
    narrow = Group(gn, qn, npeak, nsum, nwidth, 256)
    wide = Group(gw, qw, wpeak, wsum, wwidth, 256)
    narrow.start()
    wide.start()
    groups = (narrow, wide)
    for copy in loads[2:]:
        copy.wait()

    def absorb(piece, *slots):
        for slot in slots:
            to_mate(piece, slot).wait_recv()
        groups[piece].absorb(slots)

    def pass_on(piece, step):
        @pl.when(step < half)
        def _():
            arrive(piece, step)
            if piece == 1:
                ring(piece, 0, step, step + 1).start()
            else:

                @pl.when(step + 1 < half)
                def _():
                    ring(piece, 0, step, step + 1).start()

            to_mate(piece, step).start()
            arrive(piece, half + step)
            if piece == 0:
                ring(piece, 1, half + step, jnp.where(step + 1 < half, half + step + 1, half)).start()
            else:

                @pl.when(step + 1 < half)
                def _():
                    ring(piece, 1, half + step, half + step + 1).start()

            to_mate(piece, half + step).start()

        @pl.when(step == half)
        def _():
            arrive(piece, half)
            to_mate(piece, half).start()

    absorb(0, 0)
    absorb(1, 0)
    early = half // 2

    def turn(step, carry):
        pass_on(0, step)

        @pl.when(step > 1)
        def _():
            absorb(1, step - 1, half + step - 1)

        pass_on(1, step)

        @pl.when(lax.rem(step, 2) == 0)
        def _():
            serve_share(step // 2)

        absorb(0, step, half + step)
        return carry

    lax.fori_loop(1, half, turn, 0)
    pass_on(0, jnp.int32(half))
    absorb(1, half - 1, chips - 1)
    pass_on(1, jnp.int32(half))
    serve_share(early)
    wsend(1)
    absorb(0, half)

    def drain_keys():
        def one(step, carry):
            back = jnp.where(step == 0, 0, half + step)

            @pl.when(step < half)
            def _():
                ring(1, 0, step, step + 1).wait_send()
                ring(0, 1, back, half).wait_send()

            @pl.when(step + 1 < half)
            def _():
                ring(0, 0, step, step + 1).wait_send()
                ring(1, 1, back, half).wait_send()

            return carry

        def mates(slot, carry):
            for piece in (0, 1):
                to_mate(piece, slot).wait_send()
            return carry

        lax.fori_loop(0, half, one, 0)
        lax.fori_loop(0, chips, mates, 0)

    def drain_weights(kind):
        def one(step, carry):
            back = jnp.where(step == 0, 0, half + step)
            wring(kind, 0, 0, step, step + 1).wait_send()
            wring(kind, 1, 1, back, half).wait_send()

            @pl.when(step + 1 < half)
            def _():
                wring(kind, 1, 0, step, step + 1).wait_send()
                wring(kind, 0, 1, back, half).wait_send()

            return carry

        def mates(slot, carry):
            wmate(kind, slot).wait_send()
            if kind == 0:
                wmate(2, slot).wait_send()

                @pl.when(slot > 0)
                def _():
                    cross(slot).wait_send()

            return carry

        lax.fori_loop(0, half, one, 0)
        lax.fori_loop(0, chips, mates, 0)

    kinds = {"x": serve_share, "c": serve_cross, "d": serve_down}
    plan = ["", "", "", "x5", "", "d1", "", "x6k0", "d2c1c2c3c4", "", "x7c5", "d3", "x8", "c6", "d4c7"]

    def serve():
        hook = plan.pop(0)
        for kind, step in zip(hook[::2], hook[1::2]):
            if kind == "k":
                drain_keys()
            else:
                kinds[kind](int(step))

    absorb(1, half)

    narrow_rows, wide_rows = narrow.finished(), wide.finished()
    low = 0
    for result, width in ((narrow_rows, nwidth), (wide_rows, wwidth)):
        for head in range(result.shape[0] // tokens):
            attn[:, low : low + width] = result[head * tokens : (head + 1) * tokens]
            low += width

    chunk = part.shape[3]

    def emit(c):
        terms = nn(attn[...], projection[:, c * chunk : (c + 1) * chunk]).astype(BF16)
        part[c] = terms.reshape(part.shape[1:])

    def dest(j):
        return {"tp": j}

    sums = {}
    reduce_scatter(
        dest,
        (part, relay, pair, direct),
        scatter_sems[:6],
        "tp",
        emit,
        serve,
        sums.__setitem__,
        CHUNKS,
    )
    attended = jnp.concatenate([sums[c] for c in range(CHUNKS)], axis=1)
    kept = residual[...].astype(F32) + attended.astype(F32)
    stream[...] = kept
    scale = lax.rsqrt(jnp.mean(kept * kept, axis=-1, keepdims=True) + EPS)
    normed = (kept * scale * mgain[...]).astype(BF16)
    split = rows.shape[3]
    rows[0, tp] = normed[:, :split]
    rows[1, tp] = normed[:, split:]

    def gather(h, way, owner):
        return pltpu.make_async_remote_copy(
            rows.at[h, owner],
            rows.at[h, owner],
            ag_send.at[h, way, owner],
            ag_recv.at[h, owner],
            {"tp": right if way == 0 else left},
            MESH,
        )

    gather(0, 0, tp).start()
    gather(1, 1, tp).start()
    gather(1, 0, tp).start()
    gather(0, 1, tp).start()
    serve()
    gather(0, 0, left).wait_recv()
    gather(0, 0, left).start()
    serve()
    gather(1, 0, right).wait_recv()
    gather(1, 1, right).start()
    serve()
    for h, owner in ((1, left), (0, right), (0, across), (1, across)):
        gather(h, 0, owner).wait_recv()
        serve()

    def settle(kind):
        def one(slot, carry):
            wmate(kind, slot).wait_recv()
            return carry

        lax.fori_loop(0, chips, one, 0)

    serve_cross(half)
    serve_down(half - 3)
    settle(0)
    settle(2)
    units = hidden.shape[1]
    model = weights.shape[1] * weights.shape[2]
    def visit(i, carry):
        span = pl.ds(pl.multiple_of(i * 128, 128), 128)
        both = [weights[k, :, :, span].reshape(model, 128) for k in (0, 1)]
        both = jnp.concatenate(both, axis=1)
        product = nn(rows[0].reshape(tokens, split), both[:split])
        product += nn(rows[1].reshape(tokens, split), both[split:])
        gate, up = product[:, :128], product[:, 128:]
        hidden[:, span] = (gate / (1.0 + jnp.exp(-gate)) * up).astype(BF16)
        return carry

    blocks = units // 128
    early_blocks = 2 * blocks // 3
    lax.fori_loop(0, early_blocks, visit, 0)
    serve_down(half - 2)
    lax.fori_loop(early_blocks, blocks, visit, 0)
    due = {2: half - 1, 5: half}

    depth = weights.shape[2]
    arrival = [0]
    for k in range(1, half):
        arrival += [k, half + k]
    arrival.append(half)
    per = part2.shape[3] // (2 * depth)

    def columns(slot):
        return pl.ds(pl.multiple_of(depth * (source(slot) - core), 2 * depth), 2 * depth)

    def emit_down(c):
        mine = arrival[c * per : (c + 1) * per]
        if c in due:
            serve_down(due[c])
        pieces = []
        for slot in mine:
            wmate(1, slot).wait_recv()
            both = weights[2, pl.ds(source(slot) - core, 2)]
            pieces.append(both.reshape(2 * depth, units))
        terms = nt(hidden[...], jnp.concatenate(pieces, axis=0)).astype(BF16)
        part2[c] = terms.reshape(part2.shape[1:])

    def finish_down(c, total):
        for k, slot in enumerate(arrival[c * per : (c + 1) * per]):
            span = columns(slot)
            piece = total[:, k * 2 * depth : (k + 1) * 2 * depth]
            out[:, span] = (stream[:, span] + piece.astype(F32)).astype(BF16)

    reduce_scatter(
        dest,
        (part2, relay2, pair2, direct2),
        scatter_sems[6:],
        "tp",
        emit_down,
        lambda: None,
        finish_down,
        3,
    )
    drain_weights(0)

    for h, way, owner in ((0, 0, tp), (1, 1, tp), (1, 0, tp), (0, 1, tp), (0, 0, left), (1, 1, right)):
        gather(h, way, owner).wait_send()

    drain_weights(1)


def scatter_scratch(chunks, owners, owned, model):
    chunk = model // chunks
    return [
        pltpu.VMEM((chunks, owners, owned, chunk), BF16),
        pltpu.VMEM((chunks, owned, chunk), BF16),
        pltpu.VMEM((chunks, 2, owned, chunk), BF16),
        pltpu.VMEM((chunks, owned, chunk), BF16),
    ]


def local(
    chips,
    residual_in,
    narrow_query_rows,
    wide_query_rows,
    narrow_key_value,
    wide_key_value,
    narrow_norm_gains,
    wide_norm_gains,
    out_narrow,
    out_wide,
    mixer_gain,
    mixer_gate,
    mixer_up,
    mixer_down,
):
    tokens = narrow_query_rows.shape[0]
    owned, model = residual_in.shape
    owners = tokens // owned
    nkv = narrow_key_value.reshape(tokens, -1)
    wkv = wide_key_value.reshape(tokens, -1)
    nwidth, wwidth = nkv.shape[1] // 2, wkv.shape[1] // 2
    nrows = narrow_query_rows.shape[1] // nwidth * tokens
    wrows = wide_query_rows.shape[1] // wwidth * tokens
    depth, units = mixer_gate.shape
    joint = out_narrow.shape[0] + out_wide.shape[0]
    vmem = pl.BlockSpec(memory_space=pltpu.VMEM)
    hbm = pl.BlockSpec(memory_space=pl.ANY)
    VMEM, DMA = pltpu.VMEM, pltpu.SemaphoreType.DMA

    return pl.pallas_call(
        functools.partial(layer_kernel, chips),
        out_shape=jax.ShapeDtypeStruct((owned, model), BF16),
        in_specs=[vmem] * 9 + [hbm] * 5,
        out_specs=vmem,
        scratch_shapes=[
            VMEM((tokens, 2 * nwidth), F32),
            VMEM((tokens, 2 * wwidth), F32),
            VMEM((3, 2 * chips, depth, units), BF16),
            VMEM((chips, 2, tokens, nkv.shape[1]), BF16),
            VMEM((chips, 2, tokens, wkv.shape[1]), BF16),
            VMEM((nrows, nkv.shape[1]), BF16),
            VMEM((wrows, wwidth), BF16),
            VMEM((1, nrows), F32),
            VMEM((1, wrows), F32),
            VMEM((PAD + nwidth, nrows), F32),
            VMEM((PAD + wwidth, wrows), F32),
            VMEM((tokens, joint), BF16),
            VMEM((joint, model), BF16),
            *scatter_scratch(CHUNKS, owners, owned, model),
            *scatter_scratch(LATE_CHUNKS, owners, owned, model),
            VMEM((owned, model), F32),
            VMEM((2, owners, owned, model // 2), BF16),
            VMEM((tokens, units), BF16),
            DMA((2, chips)),
            DMA((2, chips)),
            DMA((2, chips)),
            DMA((2, chips)),
            DMA((2, 2, chips)),
            DMA((2, 2, chips)),
            DMA((3, chips)),
            DMA((3, chips)),
            DMA((chips,)),
            DMA((chips,)),
            DMA((5,)),
            DMA((2, 2, owners)),
            DMA((2, owners)),
            *[DMA((CHUNKS,))] * 6,
            *[DMA((LATE_CHUNKS,))] * 6,
        ],
        compiler_params=pltpu.CompilerParams(
            collective_id=0, has_side_effects=True, vmem_limit_bytes=60 * 2**20
        ),
        name="layer",
    )(
        narrow_query_rows,
        wide_query_rows,
        nkv,
        wkv,
        narrow_norm_gains,
        wide_norm_gains,
        jnp.asarray(frequencies(wwidth, nwidth)),
        residual_in,
        mixer_gain.reshape(1, -1),
        mixer_down.T,
        out_narrow,
        out_wide,
        mixer_gate,
        mixer_up,
    )


def solution(mesh):
    placed = (
        P(("grp", "sp", "tp"), None),
        P(("grp", "sp"), "tp"),
        P(("grp", "sp"), "tp"),
        P(("grp", "sp"), "tp", None),
        P(("grp", "sp"), "tp", None),
        P(),
        P(),
        P("tp", None),
        P("tp", None),
        P(),
        P("sp", "tp"),
        P("sp", "tp"),
        P("tp", "sp"),
    )
    return jax.shard_map(
        functools.partial(local, mesh.shape["sp"] // 2),
        mesh=mesh,
        in_specs=placed,
        out_specs=P(("grp", "sp", "tp"), None),
        check_vma=False,
    )
```
